32 devices in a mesh: ep: 32 (over z, y, x, core).
Axes of the slice: x: 2, y: 2, z: 4, core: 2. Of those that a mesh axis runs over, the one named last changes fastest.
Arguments:
- hidden: bfloat16 [1024, 2048], P('ep'), may hold values from -6 to 6
- cache_keys: bfloat16 [1024, 1024, 128], P('ep'), may hold values from -512 to 512
- cache_values: bfloat16 [1024, 1024, 128], P('ep'), may hold values from -6 to 6
- lengths: int32 [1024], P('ep'), may hold values from 1 to 1024
- first_gain: float32 [2048], replicated, may hold values from 0.1 to 1.9
- query_weight: bfloat16 [2048, 1024], replicated, may hold values from -0.125 to 0.125
- key_weight: bfloat16 [2048, 128], replicated, may hold values from -0.125 to 0.125
- value_weight: bfloat16 [2048, 128], replicated, may hold values from -0.125 to 0.125
- mixing: float32 [8], replicated, may hold values from 0.3 to 0.8
- head_gain: float32 [128], replicated, may hold values from 0.1 to 1.9
- out_weight: bfloat16 [1024, 2048], replicated, may hold values from -0.1875 to 0.1875
- second_gain: float32 [2048], replicated, may hold values from 0.1 to 1.9
- routes: int32 [1024, 4], P('ep'), may hold values from 0 to 15, as said below
- route_weight: float32 [1024, 4], P('ep'), may hold values from 0.05 to 1
- expert_gate: bfloat16 [32, 2048, 256], P('ep'), may hold values from -0.125 to 0.125
- expert_up: bfloat16 [32, 2048, 256], P('ep'), may hold values from -0.125 to 0.125
- expert_down: bfloat16 [32, 256, 2048], P('ep'), may hold values from -0.25 to 0.25
Outputs:
- layer_out: bfloat16 [1024, 2048], P('ep')
- new_key: bfloat16 [1024, 128], P('ep')
- new_value: bfloat16 [1024, 128], P('ep')
The draws below stay inside these ranges and needn't reach their ends.
Inputs may be any that keep to these rules, and one draw needn't show every extreme that they name: `routes`: each row names 4 different experts of one group, that is of one block of 4 consecutive numbers. Among the rows of one device, two rows name the same set of experts or disjoint sets, and no expert is named by more than 16 rows; one and the same expert is named by exactly 16 rows on every device.
All inputs are finite; a program needn't handle non-finite values.
Results may differ from the reference program's by a relative error of at most 0.025.
Values may be sent and summed in bfloat16 or wider, within the bound.
A program may use at most 128 MiB of HBM per device.

```python
import math
import jax
import jax.numpy as jnp
from jax import lax

D = 2048
HEADS = 8
DK = 64
DV = 128
D_EXPERT = 512
GROUPS = 4
EXP_SPLIT = 2
TOP_K = 4
SEQ_DEV = 32
LEN = 1024
TOKENS = 1024
EXPERTS = 16
EXP_GROUP = 4
CAP = 16


def draw_cache_keys(key, part):
    first = jax.random.fold_in(jax.random.fold_in(key, 3), 0)
    base = 1.8 * jnp.clip(jax.random.normal(first, (TOKENS, LEN, 2 * DK), jnp.float32), -6.0, 6.0)
    return base.astype(jnp.bfloat16)


def draw_routes(key, part):
    blocks = TOKENS // SEQ_DEV
    sets_group = EXP_GROUP // TOP_K
    set_count = EXPERTS // TOP_K
    tickets = set_count * CAP
    base = jax.random.fold_in(key, 7)
    star = jax.random.randint(jax.random.fold_in(base, 1), (), 0, EXPERTS).astype(jnp.int32)
    star_group = star // EXP_GROUP
    star_inner = star % EXP_GROUP

    def one_block(block_key):
        key_perm, key_order, key_rows = jax.random.split(block_key, 3)
        inner = jax.vmap(lambda part_key: jax.random.permutation(part_key, EXP_GROUP))(jax.random.split(key_perm, GROUPS)).astype(jnp.int32)
        members = inner + (jnp.arange(GROUPS, dtype=jnp.int32) * EXP_GROUP)[:, None]
        members = members.reshape(set_count, TOP_K)
        star_slot = jnp.sum(jnp.where(inner[star_group] == star_inner, jnp.arange(EXP_GROUP, dtype=jnp.int32), 0))
        star_set = star_group * sets_group + star_slot // TOP_K
        ticket_set = jnp.arange(tickets, dtype=jnp.int32) // CAP
        ranks = jax.random.permutation(key_order, tickets).astype(jnp.int32)
        sort_key = jnp.where(ticket_set == star_set, ranks - tickets, ranks)
        chosen = ticket_set[jnp.argsort(sort_key)[:SEQ_DEV]]
        rows = members[chosen]
        shuffle = jax.vmap(lambda row_key: jax.random.permutation(row_key, TOP_K))(jax.random.split(key_rows, SEQ_DEV)).astype(jnp.int32)
        return jnp.take_along_axis(rows, shuffle, axis=1)
    block_keys = jax.random.split(jax.random.fold_in(base, 2), blocks)
    return jax.vmap(one_block)(block_keys).reshape(TOKENS, TOP_K).astype(jnp.int32)


def place_ends(array, key, low, largest):
    dims = array.shape
    index_at = [jax.random.randint(jax.random.fold_in(key, axis), (), 0, dims[axis]) for axis in range(len(dims))]
    array = array.at[tuple(index_at)].set(low)
    longest = dims.index(max(dims))
    index_at[longest] = (index_at[longest] + 1) % dims[longest]
    return array.at[tuple(index_at)].set(largest)


def block_levels(own_key, shape, cuts, low, largest):
    level, own = 1.0, jax.random.fold_in(own_key, 6)
    for axis_at, shards_of in cuts:
        heights = jnp.exp(jax.random.uniform(jax.random.fold_in(own, axis_at), (shards_of,), jnp.float32, low / len(cuts), largest / len(cuts)))
        level = level * jnp.repeat(heights, shape[axis_at] // shards_of).reshape([-1 if axis == axis_at else 1 for axis in range(len(shape))])
    return level


def normal_values(stream_key, dims, deviation, limit, cuts=(), kind=jnp.bfloat16):
    entries = deviation * jax.random.normal(stream_key, dims, jnp.float32)
    if cuts:
        entries = entries * block_levels(stream_key, dims, cuts, -0.22, 0.18)
    return jnp.clip(entries, -limit, limit).astype(kind)


def setup_inputs(seed: int = 0) -> dict:
    key_of = jax.random.split(jax.random.key(seed), 18)
    hidden = normal_values(key_of[0], (TOKENS, D), 1.0, 6.0, ((0, 32),))
    cache_keys = draw_cache_keys(jax.random.fold_in(key_of[17], 71), 0)
    cache_values = normal_values(key_of[2], (TOKENS, LEN, DV), 1.0, 6.0, ((0, 32),))
    lengths = place_ends(jax.random.randint(key_of[3], (TOKENS,), 1, LEN + 1), jax.random.fold_in(key_of[3], 1), 1, LEN).astype(jnp.int32)
    first_gain = jnp.clip(1.0 + 0.18 * jax.random.normal(key_of[4], (D,), jnp.float32), 0.1, 1.9)
    query_weight = normal_values(key_of[5], (D, HEADS * 2 * DK), D ** -0.5, 0.125)
    key_weight = normal_values(key_of[6], (D, 2 * DK), D ** -0.5, 0.125)
    value_weight = normal_values(key_of[7], (D, DV), D ** -0.5, 0.125)
    mixing = jnp.clip(jax.random.uniform(key_of[8], (HEADS,), jnp.float32, 0.3, 0.8), 0.3, 0.8)
    head_gain = jnp.clip(1.0 + 0.18 * jax.random.normal(key_of[9], (DV,), jnp.float32), 0.1, 1.9)
    out_weight = normal_values(key_of[10], (HEADS * DV, D), (HEADS * DV) ** -0.5, 0.1875)
    second_gain = jnp.clip(1.0 + 0.18 * jax.random.normal(key_of[11], (D,), jnp.float32), 0.1, 1.9)
    routes = draw_routes(jax.random.fold_in(key_of[17], 71), 0)
    route_weight = jnp.clip(jnp.exp(math.log(1.0) - 2.9957323 * jax.random.uniform(key_of[13], (TOKENS, TOP_K), jnp.float32) ** block_levels(key_of[13], (TOKENS, TOP_K), ((0, 32),), -0.2, 0.2)), 0.05, 1.0)
    expert_gate = normal_values(key_of[14], (EXPERTS * EXP_SPLIT, D, D_EXPERT // EXP_SPLIT), D ** -0.5, 0.125, ((0, 32),))
    expert_up = normal_values(key_of[15], (EXPERTS * EXP_SPLIT, D, D_EXPERT // EXP_SPLIT), D ** -0.5, 0.125, ((0, 32),))
    expert_down = normal_values(key_of[16], (EXPERTS * EXP_SPLIT, D_EXPERT // EXP_SPLIT, D), D_EXPERT ** -0.5, 0.25, ((0, 32),))
    return {"hidden": hidden, "cache_keys": cache_keys, "cache_values": cache_values, "lengths": lengths, "first_gain": first_gain, "query_weight": query_weight, "key_weight": key_weight, "value_weight": value_weight, "mixing": mixing, "head_gain": head_gain, "out_weight": out_weight, "second_gain": second_gain, "routes": routes, "route_weight": route_weight, "expert_gate": expert_gate, "expert_up": expert_up, "expert_down": expert_down}


epsilon = 1e-06

def root_scale(rows, gain):
    values = rows.astype(jnp.float32)
    factor = lax.rsqrt(lax.optimization_barrier(jnp.mean(values * values, axis=-1, keepdims=True)) + epsilon)
    return values * factor * gain

def slot_tables(routes, experts, capacity):
    count, picks = routes.shape
    flat = routes.reshape(count * picks)
    indicator = (flat[:, None] == jnp.arange(experts, dtype=jnp.int32)[None, :]).astype(jnp.int32)
    before = jnp.cumsum(indicator, axis=0) - indicator
    place = lax.optimization_barrier(jnp.sum(before * indicator, axis=1))
    target = flat * capacity + place
    slots = jnp.arange(experts * capacity, dtype=jnp.int32)
    match = target[None, :] == slots[:, None]
    return match.reshape(experts * capacity, count, picks)

def attend(query, new_key, new_value, cache_keys, cache_values, lengths, mixing):
    count = query.shape[0]
    span = cache_keys.shape[1]
    queries = query.reshape(count, HEADS, 2, DK)
    keys = cache_keys.reshape(count, span, 2, DK)
    scores = jnp.einsum('shmd,slmd->shml', queries.astype(jnp.float32), keys.astype(jnp.float32)) * DK ** (-0.5)
    own_scores = jnp.einsum('shmd,smd->shm', queries.astype(jnp.float32), new_key.reshape(count, 2, DK).astype(jnp.float32)) * DK ** (-0.5)
    valid = jnp.arange(span, dtype=jnp.int32)[None, :] < lengths[:, None]
    scores = jnp.where(valid[:, None, None, :], scores, -jnp.inf)
    highest = jnp.maximum(lax.optimization_barrier(jnp.max(scores, axis=-1)), own_scores)
    weights = jnp.exp(scores - highest[..., None])
    own_weights = jnp.exp(own_scores - highest)
    total = lax.optimization_barrier(jnp.sum(weights, axis=-1)) + own_weights
    weights = weights / total[..., None]
    own_weights = own_weights / total
    contrast = (weights[:, :, 0] - mixing[None, :, None] * weights[:, :, 1]).astype(jnp.bfloat16)
    own_contrast = (own_weights[:, :, 0] - mixing[None, :] * own_weights[:, :, 1]).astype(jnp.bfloat16)
    mixed = jnp.einsum('shl,sle->she', contrast.astype(jnp.float32), cache_values.astype(jnp.float32))
    return mixed + own_contrast.astype(jnp.float32)[..., None] * new_value.astype(jnp.float32)[:, None, :]

def head_norm(mixed, head_gain):
    factor = lax.rsqrt(lax.optimization_barrier(jnp.mean(mixed * mixed, axis=-1, keepdims=True)) + epsilon)
    scaled = mixed * factor * head_gain
    return scaled.reshape(mixed.shape[0], HEADS * DV).astype(jnp.bfloat16)

def reference(hidden, cache_keys, cache_values, lengths, first_gain, query_weight, key_weight, value_weight, mixing, head_gain, out_weight, second_gain, routes, route_weight, expert_gate, expert_up, expert_down):
    normed = root_scale(hidden, first_gain).astype(jnp.bfloat16)
    query = jnp.dot(normed, query_weight, preferred_element_type=jnp.float32).astype(jnp.bfloat16)
    new_key = jnp.dot(normed, key_weight, preferred_element_type=jnp.float32).astype(jnp.bfloat16)
    new_value = jnp.dot(normed, value_weight, preferred_element_type=jnp.float32).astype(jnp.bfloat16)
    mixed = attend(query, new_key, new_value, cache_keys, cache_values, lengths, mixing)
    head_rows = head_norm(mixed, head_gain)
    update = jnp.dot(head_rows, out_weight, preferred_element_type=jnp.float32)
    residual = (hidden.astype(jnp.float32) + update).astype(jnp.bfloat16)
    expert_input = root_scale(residual, second_gain).astype(jnp.bfloat16)
    blocks = TOKENS // SEQ_DEV
    match = jax.vmap(lambda block: slot_tables(block, EXPERTS, CAP))(routes.reshape(blocks, SEQ_DEV, TOP_K))
    pick = lax.optimization_barrier(jnp.sum(match.astype(jnp.float32), axis=3))
    packed = jnp.einsum('bjs,bsd->bjd', pick, expert_input.reshape(blocks, SEQ_DEV, D).astype(jnp.float32))
    packed = packed.astype(jnp.bfloat16).reshape(blocks, EXPERTS, CAP, D)

    def one_expert(index):
        rows = lax.dynamic_index_in_dim(packed, index, 1, keepdims=False).reshape(blocks * CAP, D)
        summed = jnp.zeros((blocks * CAP, D), jnp.float32)
        for share in range(EXP_SPLIT):
            part = index * EXP_SPLIT + share
            gate = jnp.dot(rows, expert_gate[part], preferred_element_type=jnp.float32)
            upper = jnp.dot(rows, expert_up[part], preferred_element_type=jnp.float32)
            inner = (jax.nn.silu(gate) * upper).astype(jnp.bfloat16)
            result = jnp.dot(inner, expert_down[part], preferred_element_type=jnp.float32).astype(jnp.bfloat16)
            summed = summed + result.astype(jnp.float32)
        return summed.reshape(blocks, CAP, D)
    outputs = lax.map(one_expert, jnp.arange(EXPERTS, dtype=jnp.int32))
    outputs = jnp.moveaxis(outputs, 0, 1).reshape(blocks, EXPERTS * CAP, D)
    weighting = lax.optimization_barrier(jnp.sum(jnp.where(match, route_weight.reshape(blocks, 1, SEQ_DEV, TOP_K), 0.0), axis=3))
    routed = jnp.einsum('bjs,bjd->bsd', weighting, outputs, precision=lax.Precision.HIGHEST)
    layer_out = (residual.astype(jnp.float32) + routed.reshape(TOKENS, D)).astype(jnp.bfloat16)
    return (layer_out, new_key, new_value)
```

```python
import functools
import math

import jax
import jax.numpy as jnp
from jax import lax
from jax.experimental import pallas as pl
from jax.experimental.pallas import tpu as pltpu
from jax.sharding import PartitionSpec as P

D = 2048
HEADS = 8
DK = 64
DV = 128
EXP_SPLIT = 2
TOP_K = 4
GROUPS = 4
SIDE = 64


epsilon = 1e-06


def column(row):
    size = row.shape[1]
    down = lax.broadcasted_iota(jnp.int32, (size, size), 0)
    across = lax.broadcasted_iota(jnp.int32, (size, size), 1)
    return jnp.sum(jnp.where(down == across, row, jnp.zeros_like(row)), axis=1, keepdims=True)


def front_kernel(height, each, lengths, hidden, keys, values, first_gain, query_weight, key_weight, value_weight,
                 mixing, head_gain, out_weight, second_gain, routes, route_weight,
                 residual, new_key, new_value, pack, unpick,
                 key_buf, value_buf, query_buf, kv_buf, out_buf, queries, heads, fresh, contrast, owns, sems, key_sems, value_sems):
    count, width = hidden.shape
    span = keys.shape[1]
    groups = key_sems.shape[0]
    batch = count // groups
    low = jnp.bfloat16
    loads = [
        pltpu.make_async_copy(query_weight, query_buf, sems.at[0]),
        pltpu.make_async_copy(key_weight, kv_buf.at[0], sems.at[1]),
        pltpu.make_async_copy(value_weight, kv_buf.at[1], sems.at[2]),
        pltpu.make_async_copy(out_weight, out_buf, sems.at[3]),
    ]

    def fetch(source, target, flags, step):
        at = pl.ds(step * batch, batch)
        return pltpu.make_async_copy(source.at[at], target.at[at], flags.at[step])

    def fetch_keys(step):
        return fetch(keys, key_buf, key_sems, step)

    def fetch_values(step):
        return fetch(values, value_buf, value_sems, step)

    for copy in loads[:3]:
        copy.start()

    def begin_keys(step, carry):
        fetch_keys(step).start()
        return carry

    def begin_values(step, carry):
        fetch_values(step).start()
        return carry

    lax.fori_loop(0, groups, begin_keys, 0)
    lax.fori_loop(0, groups, begin_values, 0)
    loads[3].start()

    entry = hidden[...].astype(jnp.float32)
    factor = lax.rsqrt(jnp.mean(entry * entry, axis=-1, keepdims=True) + epsilon)
    normed = (entry * factor * first_gain[...]).astype(low)
    lane = lax.broadcasted_iota(jnp.int32, (count, 2 * DK), 1)
    loads[0].wait()
    query = jnp.dot(normed, query_buf[...], preferred_element_type=jnp.float32)
    query = query.astype(low).astype(jnp.float32)
    for head in range(HEADS):
        block = query[:, head * 2 * DK : (head + 1) * 2 * DK]
        queries[:, head, :] = jnp.where(lane < DK, block, 0.0)
        queries[:, HEADS + head, :] = jnp.where(lane < DK, 0.0, block)
    for index, result in ((0, new_key), (1, new_value)):
        loads[1 + index].wait()
        made = jnp.dot(normed, kv_buf[index], preferred_element_type=jnp.float32).astype(low)
        result[...] = made
        fresh[index] = made.astype(jnp.float32)

    position = lax.broadcasted_iota(jnp.int32, (1, span), 1)

    mixes = column(mixing[...])

    def weigh(step, carry):
        fetch_keys(step).wait()
        for offset in range(batch):
            s = step * batch + offset
            wide = queries[s]
            own_key = fresh[0, pl.ds(s, 1), :]
            scores = lax.dot_general(
                wide.astype(low),
                key_buf[s],
                (((1,), (1,)), ((), ())),
                preferred_element_type=jnp.float32,
            ) * DK ** (-0.5)
            own = jnp.sum(wide * own_key, axis=-1, keepdims=True) * DK ** (-0.5)
            scores = jnp.where(position < lengths[s], scores, -jnp.inf)
            highest = jnp.maximum(jnp.max(scores, axis=-1, keepdims=True), own)
            weights = jnp.exp(scores - highest)
            own = jnp.exp(own - highest)
            inverse = 1.0 / (jnp.sum(weights, axis=-1, keepdims=True) + own)
            first, second = inverse[:HEADS], inverse[HEADS:] * mixes
            contrast[s] = weights[:HEADS] * first - weights[HEADS:] * second
            own = (own[:HEADS] * first - own[HEADS:] * second).astype(low).astype(jnp.float32)
            owns[s] = own * fresh[1, pl.ds(s, 1), :]
        return carry

    lax.fori_loop(0, groups, weigh, 0)

    def mix(step, carry):
        fetch_values(step).wait()
        for offset in range(batch):
            s = step * batch + offset
            mixed = jnp.dot(contrast[s].astype(low), value_buf[s], preferred_element_type=jnp.float32)
            mixed += owns[s]
            scale = lax.rsqrt(jnp.mean(mixed * mixed, axis=-1, keepdims=True) + epsilon)
            heads[s] = mixed * scale * head_gain[...]
        return carry

    lax.fori_loop(0, groups, mix, 0)

    joined = jnp.concatenate([heads[:, head, :] for head in range(HEADS)], axis=1).astype(low)
    loads[3].wait()
    update = jnp.dot(joined, out_buf[...], preferred_element_type=jnp.float32)
    kept = (hidden[...].astype(jnp.float32) + update).astype(low)
    residual[...] = kept
    kept = kept.astype(jnp.float32)
    factor = lax.rsqrt(jnp.mean(kept * kept, axis=-1, keepdims=True) + epsilon)
    inputs = (kept * factor * second_gain[...]).astype(low)

    group = column(routes[:1, :]) // each
    down = lax.broadcasted_iota(jnp.int32, (count, count), 0)
    across = lax.broadcasted_iota(jnp.int32, (count, count), 1)
    other = routes[:1, :] // each
    before = jnp.where((group == other) & (across < down), 1, 0)
    target = group * height + jnp.sum(before, axis=1, keepdims=True)
    slots = GROUPS * height
    chosen = target == lax.broadcasted_iota(jnp.int32, (count, slots), 1)
    chosen = jnp.where(chosen, 1.0, 0.0).astype(low)
    unpick[...] = chosen
    place = lax.broadcasted_iota(jnp.int32, (count, SIDE), 1)
    scale = jnp.zeros((count, SIDE), jnp.float32)
    for k in range(routes.shape[0]):
        inside = column(routes[k : k + 1, :]) - group * each
        scale += jnp.where(place == inside, column(route_weight[k : k + 1, :]), 0.0)
    high = scale.astype(low)
    side = jnp.concatenate([high, (scale - high.astype(jnp.float32)).astype(low)], axis=1)
    turned = (((0,), (0,)), ((), ()))
    packed = lax.dot_general(chosen, inputs, turned, preferred_element_type=jnp.float32)
    pack[:, :, :width] = packed.astype(low).reshape(GROUPS, height, width)
    packed = lax.dot_general(chosen, side, turned, preferred_element_type=jnp.float32)
    pack[:, :, width:] = packed.astype(low).reshape(GROUPS, height, 2 * SIDE)


def run_front(arrays, height, each):
    (hidden, cache_keys, cache_values, lengths, first_gain, query_weight, key_weight, value_weight,
     mixing, head_gain, out_weight, second_gain, routes, route_weight) = arrays
    count, width = hidden.shape
    low = jnp.bfloat16
    vmem = pl.BlockSpec(memory_space=pltpu.VMEM)
    anywhere = pl.BlockSpec(memory_space=pl.ANY)
    batch = math.gcd(count, 16)
    groups = count // batch
    slots = GROUPS * height
    span = cache_keys.shape[1]
    flops = 2 * count * (2 * query_weight.size + 2 * key_weight.size + 24 * span * DV)
    moved = 2 * (cache_keys.size + cache_values.size + 2 * query_weight.size)
    return pl.pallas_call(
        functools.partial(front_kernel, height, each),
        out_shape=(
            jax.ShapeDtypeStruct((count, width), low),
            jax.ShapeDtypeStruct((count, 2 * DK), low),
            jax.ShapeDtypeStruct((count, DV), low),
            jax.ShapeDtypeStruct((GROUPS, height, width + 2 * SIDE), low),
            jax.ShapeDtypeStruct((count, slots), low),
        ),
        in_specs=[
            pl.BlockSpec(memory_space=pltpu.SMEM), vmem, anywhere, anywhere, vmem, anywhere,
            anywhere, anywhere, vmem, vmem, anywhere, vmem, vmem, vmem,
        ],
        out_specs=(vmem,) * 5,
        scratch_shapes=[
            pltpu.VMEM(cache_keys.shape, low),
            pltpu.VMEM(cache_values.shape, low),
            pltpu.VMEM(query_weight.shape, low),
            pltpu.VMEM((2, *key_weight.shape), low),
            pltpu.VMEM(out_weight.shape, low),
            pltpu.VMEM((count, 2 * HEADS, 2 * DK), jnp.float32),
            pltpu.VMEM((count, HEADS, DV), jnp.float32),
            pltpu.VMEM((2, count, DV), jnp.float32),
            pltpu.VMEM((count, HEADS, span), jnp.float32),
            pltpu.VMEM((count, HEADS, DV), jnp.float32),
            pltpu.SemaphoreType.DMA((4,)),
            pltpu.SemaphoreType.DMA((groups,)),
            pltpu.SemaphoreType.DMA((groups,)),
        ],
        compiler_params=pltpu.CompilerParams(vmem_limit_bytes=63 * 1024 * 1024),
        cost_estimate=pl.CostEstimate(flops=flops, bytes_accessed=moved, transcendentals=0),
        name="front",
    )(
        lengths, hidden, cache_keys, cache_values, first_gain.reshape(1, -1), query_weight,
        key_weight, value_weight, mixing.reshape(1, -1), head_gain.reshape(1, -1), out_weight,
        second_gain.reshape(1, -1), routes.T, route_weight.T,
    )


def moe_kernel(dims, pack, gate_own, up_own, down_own, gate_other, up_other, down_other, residual, unpick, out,
               rows, part, first_a, send_a, second_a, first_b, send_b, second_b, final, back,
               gate, up, down, send_sems, recv_sems, local_sems):
    zs_count, ys, xs = dims
    me = lax.axis_index("ep")
    c = lax.rem(me, 2)
    x = lax.rem(me // 2, xs)
    y = lax.rem(me // (2 * xs), ys)
    z = me // (2 * xs * ys)

    def device(pz, py, px):
        return ((pz * ys + py) * xs + px) * 2 + c

    def slot(pz, py, px):
        return (pz * ys + py) * xs + px

    def zat(k):
        return lax.rem(z + k + zs_count, zs_count)

    def yat(k):
        return lax.rem(y + k + ys, ys)

    def xat(k):
        return lax.rem(x + k + xs, xs)

    used = []

    def send(src, dst, target):
        index = len(used)
        copy = pltpu.make_async_remote_copy(
            src_ref=src,
            dst_ref=dst,
            send_sem=send_sems.at[index],
            recv_sem=recv_sems.at[index],
            device_id=(target,),
            device_id_type=pl.DeviceIdType.MESH,
        )
        copy.start()
        used.append(copy)
        return copy

    weights = []
    for index, (src, dst) in enumerate(
        (
            (gate_own.at[0], gate.at[0]),
            (up_own.at[0], up.at[0]),
            (gate_other.at[0], gate.at[1]),
            (up_other.at[0], up.at[1]),
            (down_own.at[0], down.at[0]),
            (down_other.at[0], down.at[1]),
        )
    ):
        copy = pltpu.make_async_copy(src, dst, local_sems.at[index + 1])
        copy.start()
        weights.append(copy)

    barrier = pltpu.get_barrier_semaphore()
    peers = [device(zat(k), y, x) for k in range(1, zs_count)]
    peers += [device(z, yat(k), x) for k in range(1, ys)]
    peers += [device(z, y, xat(k)) for k in range(1, xs)]
    for peer in peers:
        pl.semaphore_signal(barrier, inc=1, device_id=(peer,), device_id_type=pl.DeviceIdType.MESH)
    pl.semaphore_wait(barrier, len(peers))

    mine = slot(z, y, x)
    own = pltpu.make_async_copy(pack.at[z], rows.at[mine], local_sems.at[0])
    own.start()
    arrive = {}
    for k in range(1, zs_count):
        arrive[k] = send(pack.at[zat(k)], rows.at[mine], device(zat(k), y, x))
    order = sorted(range(zs_count), key=lambda k: min(k, zs_count - k))
    along_x, along_y, pending = {}, {}, []
    for k in order:
        if k:
            arrive[k].wait_recv()
        else:
            own.wait()
        block = rows.at[slot(zat(-k), y, x)]

        def over_x():
            for j in range(1, xs):
                along_x[k, j] = send(block, block, device(z, y, xat(j)))

        def over_y():
            for i in range(1, ys):
                along_y[k, i] = send(block, block, device(z, yat(i), x))

        for step in (over_x, over_y) if k % 2 == 0 else (over_y, over_x):
            step()
    for k in order:
        pz = zat(-k)
        if k % 2 == 0:
            for j in range(1, xs):
                along_x.pop((k, j)).wait_recv()
                block = rows.at[slot(pz, y, xat(-j))]
                for i in range(1, ys):
                    pending.append(send(block, block, device(z, yat(i), x)))
        else:
            for i in range(1, ys):
                along_y.pop((k, i)).wait_recv()
                block = rows.at[slot(pz, yat(-i), x)]
                for j in range(1, xs):
                    pending.append(send(block, block, device(z, y, xat(j))))
    for copy in weights[:4]:
        copy.wait()
    for copy in (*along_x.values(), *along_y.values(), *pending):
        copy.wait_recv()
    for copy in weights[4:]:
        copy.wait()

    slots, height, width = rows.shape
    depth = part.shape[2]
    chosen = y * xs + x
    batch = max(1, min(slots, 256 // height))

    def apply(step, carry):
        at = pl.ds(step * batch, batch)
        flat = rows[at, :, :depth].reshape(batch * height, depth)
        side = rows[at, :, depth:].reshape(batch * height, width - depth).astype(jnp.float32)
        lane = lax.broadcasted_iota(jnp.int32, side.shape, 1)
        hit = lax.rem(lane, (width - depth) // 2) == chosen
        scale = jnp.sum(jnp.where(hit, side, 0.0), axis=1, keepdims=True)
        inner = []
        for half in range(2):
            left = jnp.dot(flat, gate[half], preferred_element_type=jnp.float32)
            right = jnp.dot(flat, up[half], preferred_element_type=jnp.float32)
            inner.append((left / (1.0 + jnp.exp(-left)) * right).astype(jnp.bfloat16))
        tile = 512
        for start in range(0, depth, tile):
            cols = slice(start, start + tile)
            total = jnp.dot(inner[0], down[0, :, cols], preferred_element_type=jnp.float32)
            total += jnp.dot(inner[1], down[1, :, cols], preferred_element_type=jnp.float32)
            part[at, :, cols] = (total * scale).astype(part.dtype).reshape(batch, height, tile)
        return carry

    lax.fori_loop(0, slots // batch, apply, 0)

    evens = [k for k in order if k % 2 == 0]
    odds = [k for k in order if k % 2 == 1]
    waits = {}
    for k in order:
        pz = zat(-k)
        index = k // 2
        if k % 2 == 0:
            waits[k] = [
                send(
                    part.at[pl.ds(slot(pz, yat(j), 0), xs)],
                    first_a.at[index, j - 1],
                    device(z, yat(j), x),
                )
                for j in range(1, ys)
            ]
        else:
            waits[k] = [
                send(
                    part.at[slot(pz, row, xat(j))],
                    first_b.at[index, j - 1, row],
                    device(z, y, xat(j)),
                )
                for j in range(1, xs)
                for row in range(ys)
            ]
    seconds = {}
    for k in order:
        pz = zat(-k)
        index = k // 2
        for copy in waits[k]:
            copy.wait_recv()
        seconds[k] = []
        if k % 2 == 0:
            for i in range(1, xs):
                total = part[slot(pz, y, xat(i))].astype(jnp.float32)
                for j in range(1, ys):
                    total += first_a[index, j - 1, xat(i)].astype(jnp.float32)
                send_a[index, i - 1] = total.astype(send_a.dtype)
                seconds[k].append(
                    send(send_a.at[index, i - 1], second_a.at[index, i - 1], device(z, y, xat(i)))
                )
        else:
            for i in range(1, ys):
                total = part[slot(pz, yat(i), x)].astype(jnp.float32)
                for j in range(1, xs):
                    total += first_b[index, j - 1, yat(i)].astype(jnp.float32)
                send_b[index, i - 1] = total.astype(send_b.dtype)
                seconds[k].append(
                    send(send_b.at[index, i - 1], second_b.at[index, i - 1], device(z, yat(i), x))
                )
    returns = []
    for k in sorted(order, key=lambda k: (k == 0, k)):
        pz = zat(-k)
        index = k // 2
        for copy in seconds[k]:
            copy.wait_recv()
        total = part[slot(pz, y, x)].astype(jnp.float32)
        if k % 2 == 0:
            for j in range(1, ys):
                total += first_a[index, j - 1, x].astype(jnp.float32)
            for i in range(1, xs):
                total += second_a[index, i - 1].astype(jnp.float32)
        else:
            for j in range(1, xs):
                total += first_b[index, j - 1, y].astype(jnp.float32)
            for i in range(1, ys):
                total += second_b[index, i - 1].astype(jnp.float32)
        if k:
            final[k - 1] = total.astype(final.dtype)
            returns.append(send(final.at[k - 1], back.at[z], device(pz, y, x)))
        else:
            back[z] = total.astype(back.dtype)
    for copy in returns:
        copy.wait_recv()
    filled = back[...].reshape(zs_count * height, depth)
    routed = jnp.dot(unpick[...], filled, preferred_element_type=jnp.float32)
    out[...] = (residual[...].astype(jnp.float32) + routed).astype(out.dtype)
    for copy in used:
        copy.wait_send()


def run_experts(pack, own, other, residual, unpick, devices):
    zs = GROUPS
    chips = devices // (2 * zs)
    xs = math.isqrt(chips)
    ys = chips // xs
    _, height, width = pack.shape
    depth = residual.shape[1]
    slots = devices // 2
    hidden = own[0].shape[2]
    evens, odds = (zs + 1) // 2, zs // 2
    low = jnp.bfloat16
    count = (zs - 1) * 2 + zs * (xs + ys - 2) + zs * (xs - 1) * (ys - 1)
    count += evens * (xs + ys - 2) + odds * ((xs - 1) * ys + ys - 1)
    vmem = pl.BlockSpec(memory_space=pltpu.VMEM)
    anywhere = pl.BlockSpec(memory_space=pl.ANY)
    return pl.pallas_call(
        functools.partial(moe_kernel, (zs, ys, xs)),
        out_shape=jax.ShapeDtypeStruct(residual.shape, low),
        in_specs=[vmem] + [anywhere] * 6 + [vmem] * 2,
        out_specs=vmem,
        scratch_shapes=[
            pltpu.VMEM((slots, height, width), low),
            pltpu.VMEM((slots, height, depth), low),
            pltpu.VMEM((evens, max(1, ys - 1), xs, height, depth), low),
            pltpu.VMEM((evens, max(1, xs - 1), height, depth), low),
            pltpu.VMEM((evens, max(1, xs - 1), height, depth), low),
            pltpu.VMEM((odds, max(1, xs - 1), ys, height, depth), low),
            pltpu.VMEM((odds, max(1, ys - 1), height, depth), low),
            pltpu.VMEM((odds, max(1, ys - 1), height, depth), low),
            pltpu.VMEM((zs - 1, height, depth), low),
            pltpu.VMEM((zs, height, depth), low),
            pltpu.VMEM((2, depth, hidden), low),
            pltpu.VMEM((2, depth, hidden), low),
            pltpu.VMEM((2, hidden, depth), low),
            pltpu.SemaphoreType.DMA((count,)),
            pltpu.SemaphoreType.DMA((count,)),
            pltpu.SemaphoreType.DMA((7,)),
        ],
        compiler_params=pltpu.CompilerParams(
            collective_id=0, has_side_effects=True, vmem_limit_bytes=63 * 1024 * 1024
        ),
        name="experts",
    )(pack, *own, *other, residual, unpick)


def per_device(
    hidden,
    cache_keys,
    cache_values,
    lengths,
    first_gain,
    query_weight,
    key_weight,
    value_weight,
    mixing,
    head_gain,
    out_weight,
    second_gain,
    routes,
    route_weight,
    expert_gate,
    expert_up,
    expert_down,
):
    count = hidden.shape[0]
    devices = lax.axis_size("ep")
    experts = devices // EXP_SPLIT
    capacity = max(2, 2 * count * TOP_K // experts)
    height = capacity * (experts // GROUPS) // TOP_K
    arrays = (
        hidden, cache_keys, cache_values, lengths, first_gain, query_weight, key_weight, value_weight,
        mixing, head_gain, out_weight, second_gain, routes, route_weight,
    )
    residual, new_key, new_value, pack, unpick = run_front(arrays, height, experts // GROUPS)
    swap = [(index, index ^ 1) for index in range(devices)]
    own = (expert_gate, expert_up, expert_down)
    other = tuple(lax.ppermute(array, "ep", swap) for array in own)
    layer_out = run_experts(pack, own, other, residual, unpick, devices)
    return (layer_out, new_key, new_value)


def solution(mesh):
    return jax.shard_map(
        per_device,
        mesh=mesh,
        in_specs=(
            P("ep", None),
            P("ep", None, None),
            P("ep", None, None),
            P("ep"),
            P(),
            P(),
            P(),
            P(),
            P(),
            P(),
            P(),
            P(),
            P("ep", None),
            P("ep", None),
            P("ep", None, None),
            P("ep", None, None),
            P("ep", None, None),
        ),
        out_specs=(P("ep", None), P("ep", None), P("ep", None)),
        check_vma=False,
    )
```

```python
import functools
import math

import jax
import jax.numpy as jnp
from jax import lax
from jax.experimental import pallas as pl
from jax.experimental.pallas import tpu as pltpu
from jax.sharding import PartitionSpec as P

D = 2048
HEADS = 8
DK = 64
DV = 128
EXP_SPLIT = 2
TOP_K = 4
GROUPS = 4
SIDE = 64
ORDER = ('s0', 'f0', 's1', 'f1', 's2', 'f2', 's3', 'f3', 'c2', 'c3', 'e2', 'c1', 'e3', 'c0', 'e1', 'e0')
STRAIGHT = (0, 1, 2, 3)
GATHER = (0, 1, 2, 3)


epsilon = 1e-06


def column(row):
    size = row.shape[1]
    down = lax.broadcasted_iota(jnp.int32, (size, size), 0)
    across = lax.broadcasted_iota(jnp.int32, (size, size), 1)
    return jnp.sum(jnp.where(down == across, row, jnp.zeros_like(row)), axis=1, keepdims=True)


def layer_kernel(dims, height, each, lengths, hidden_in, keys, values, first_gain_in, query_weight, key_weight,
                 value_weight, mixing_in, head_gain_in, out_weight, second_gain_in, routes_in, route_weight_in,
                 gate_own, up_own, down_own,
                 out, new_key, new_value,
                 hidden, first_gain, mixing, head_gain, second_gain, routes, route_weight,
                 key_buf, value_buf, query_buf, kv_buf, out_buf, queries, heads, fresh, contrast, owns,
                 pack, side_pack, residual, rows, sides, part_a, part_b, first_a, first_b, send_a, send_b,
                 second_a, second_b, direct, final, back, gate, up, down,
                 load_sems, key_sems, value_sems, send_sems, recv_sems):
    zs, ys, xs = dims
    count, width = hidden.shape
    half = width // 2
    span = keys.shape[1]
    groups = key_sems.shape[0]
    batch = count // groups
    low = jnp.bfloat16
    me = lax.axis_index("ep")
    c = lax.rem(me, 2)
    x = lax.rem(me // 2, xs)
    y = lax.rem(me // (2 * xs), ys)
    z = me // (2 * xs * ys)

    def device(pz, py, px):
        return ((pz * ys + py) * xs + px) * 2 + c

    def zat(i):
        flip = z
        if i % 2:
            flip = flip + 1 - 2 * lax.rem(flip, 2)
        if i // 2:
            flip = lax.rem(flip + 2, 4)
        return flip

    def yat(j):
        return lax.rem(y + j + ys, ys)

    def xat(j):
        return lax.rem(x + j + xs, xs)

    used = []

    def send(src, dst, target):
        index = len(used)
        copy = pltpu.make_async_remote_copy(
            src_ref=src,
            dst_ref=dst,
            send_sem=send_sems.at[index],
            recv_sem=recv_sems.at[index],
            device_id=(target,),
            device_id_type=pl.DeviceIdType.MESH,
        )
        copy.start()
        used.append(copy)
        return copy

    others = [
        (i, j, k) for i in range(zs) for j in range(ys) for k in range(xs) if (i, j, k) != (0, 0, 0)
    ]
    sibling = me + 1 - 2 * c
    barrier = pltpu.get_barrier_semaphore()
    for i, j, k in others:
        pl.semaphore_signal(
            barrier, inc=1, device_id=(device(zat(i), yat(j), xat(k)),), device_id_type=pl.DeviceIdType.MESH
        )
    pl.semaphore_signal(barrier, inc=1, device_id=(sibling,), device_id_type=pl.DeviceIdType.MESH)

    moves = []
    for src, dst in (
        (hidden_in, hidden), (first_gain_in, first_gain), (routes_in, routes), (route_weight_in, route_weight),
        (mixing_in, mixing), (head_gain_in, head_gain), (second_gain_in, second_gain),
        (query_weight, query_buf), (key_weight, kv_buf.at[0]), (value_weight, kv_buf.at[1]),
        (out_weight, out_buf), (gate_own.at[0], gate.at[0]), (up_own.at[0], up.at[0]), (down_own.at[0], down.at[0]),
    ):
        moves.append(pltpu.make_async_copy(src, dst, load_sems.at[len(moves)]))
    small, query_move, kv_moves, out_move, own_moves = moves[:7], moves[7], moves[8:10], moves[10], moves[11:]

    def fetch(source, target, flags, step):
        at = pl.ds(step * batch, batch)
        return pltpu.make_async_copy(source.at[at], target.at[at], flags.at[step])

    def fetch_keys(step):
        return fetch(keys, key_buf, key_sems, step)

    def fetch_values(step):
        return fetch(values, value_buf, value_sems, step)

    for copy in (*small, query_move, *kv_moves):
        copy.start()

    def begin_keys(step, carry):
        fetch_keys(step).start()
        return carry

    def begin_values(step, carry):
        fetch_values(step).start()
        return carry

    lax.fori_loop(0, groups, begin_keys, 0)
    for copy in own_moves:
        copy.start()
    lax.fori_loop(0, groups, begin_values, 0)
    out_move.start()

    for copy in small:
        copy.wait()
    group = column(routes[:1, :]) // each
    down_at = lax.broadcasted_iota(jnp.int32, (count, count), 0)
    across = lax.broadcasted_iota(jnp.int32, (count, count), 1)
    other = routes[:1, :] // each
    before = jnp.where((group == other) & (across < down_at), 1, 0)
    target = group * height + jnp.sum(before, axis=1, keepdims=True)
    slots = zs * height
    chosen = target == lax.broadcasted_iota(jnp.int32, (count, slots), 1)
    chosen = jnp.where(chosen, 1.0, 0.0).astype(low)
    place = lax.broadcasted_iota(jnp.int32, (count, SIDE), 1)
    scale = jnp.zeros((count, SIDE), jnp.float32)
    for k in range(routes.shape[0]):
        inside = column(routes[k : k + 1, :]) - group * each
        scale += jnp.where(place == inside, column(route_weight[k : k + 1, :]), 0.0)
    high = scale.astype(low)
    side = jnp.concatenate([high, (scale - high.astype(jnp.float32)).astype(low)], axis=1)
    turned = (((0,), (0,)), ((), ()))
    packed = lax.dot_general(chosen, side, turned, preferred_element_type=jnp.float32)
    side_pack[...] = packed.astype(low).reshape(zs, height, 2 * SIDE)
    sides[0, y, x] = side_pack[z]

    entry = hidden[...].astype(jnp.float32)
    factor = lax.rsqrt(jnp.mean(entry * entry, axis=-1, keepdims=True) + epsilon)
    normed = (entry * factor * first_gain[...]).astype(low)
    lane = lax.broadcasted_iota(jnp.int32, (count, 2 * DK), 1)
    query_move.wait()
    query = jnp.dot(normed, query_buf[...], preferred_element_type=jnp.float32)
    query = query.astype(low).astype(jnp.float32)
    for head in range(HEADS):
        block = query[:, head * 2 * DK : (head + 1) * 2 * DK]
        queries[:, head, :] = jnp.where(lane < DK, block, 0.0)
        queries[:, HEADS + head, :] = jnp.where(lane < DK, 0.0, block)
    for index, result in ((0, new_key), (1, new_value)):
        kv_moves[index].wait()
        made = jnp.dot(normed, kv_buf[index], preferred_element_type=jnp.float32).astype(low)
        result[...] = made
        fresh[index] = made.astype(jnp.float32)

    pl.semaphore_wait(barrier, len(others) + 1)
    side_waits = {}
    for i, j, k in others:
        side_waits[i, j, k] = send(side_pack.at[zat(i)], sides.at[i, y, x], device(zat(i), yat(j), xat(k)))

    position = lax.broadcasted_iota(jnp.int32, (1, span), 1)
    mixes = column(mixing[...])

    def weigh(step, carry):
        fetch_keys(step).wait()
        for offset in range(batch):
            s = step * batch + offset
            wide = queries[s]
            own_key = fresh[0, pl.ds(s, 1), :]
            scores = lax.dot_general(
                wide.astype(low),
                key_buf[s],
                (((1,), (1,)), ((), ())),
                preferred_element_type=jnp.float32,
            ) * DK ** (-0.5)
            own = jnp.sum(wide * own_key, axis=-1, keepdims=True) * DK ** (-0.5)
            scores = jnp.where(position < lengths[s], scores, -jnp.inf)
            highest = jnp.maximum(jnp.max(scores, axis=-1, keepdims=True), own)
            weights = jnp.exp(scores - highest)
            own = jnp.exp(own - highest)
            inverse = 1.0 / (jnp.sum(weights, axis=-1, keepdims=True) + own)
            first, second = inverse[:HEADS], inverse[HEADS:] * mixes
            contrast[s] = weights[:HEADS] * first - weights[HEADS:] * second
            own = (own[:HEADS] * first - own[HEADS:] * second).astype(low).astype(jnp.float32)
            owns[s] = own * fresh[1, pl.ds(s, 1), :]
        return carry

    lax.fori_loop(0, groups, weigh, 0)

    pairs = ((gate, gate.at[0]), (up, up.at[0]), (down, down.at[0]))
    swaps = []
    for copy, (whole, mine) in zip(own_moves, pairs):
        copy.wait()
        swaps.append(send(mine, whole.at[1], sibling))

    def mix(step, carry):
        fetch_values(step).wait()
        for offset in range(batch):
            s = step * batch + offset
            mixed = jnp.dot(contrast[s].astype(low), value_buf[s], preferred_element_type=jnp.float32)
            mixed += owns[s]
            scale = lax.rsqrt(jnp.mean(mixed * mixed, axis=-1, keepdims=True) + epsilon)
            heads[s] = mixed * scale * head_gain[...]
        return carry

    lax.fori_loop(0, groups, mix, 0)

    joined = jnp.concatenate([heads[:, head, :] for head in range(HEADS)], axis=1).astype(low)
    out_move.wait()
    update = jnp.dot(joined, out_buf[...], preferred_element_type=jnp.float32)
    kept = (hidden[...].astype(jnp.float32) + update).astype(low)
    residual[...] = kept
    kept = kept.astype(jnp.float32)
    factor = lax.rsqrt(jnp.mean(kept * kept, axis=-1, keepdims=True) + epsilon)
    inputs = (kept * factor * second_gain[...]).astype(low)
    for h in range(2):
        packed = lax.dot_general(
            chosen, inputs[:, h * half : (h + 1) * half], turned, preferred_element_type=jnp.float32
        )
        pack[:, h] = packed.astype(low).reshape(zs, height, half)

    arrive, along_x, along_y, corner = {}, {}, {}, {}
    ones, twos, ends = {}, {}, {}

    def spread(i):
        if i:
            arrive[i].wait_recv()
        block = rows.at[i, y, x]
        corner[i] = []
        if i in STRAIGHT:
            for j in range(1, ys):
                for k in range(1, xs):
                    corner[i].append(send(block, block, device(z, yat(j), xat(k))))
        for j in range(1, xs):
            along_x[i, j] = send(block, block, device(z, y, xat(j)))
        for j in range(1, ys):
            along_y[i, j] = send(block, block, device(z, yat(j), x))

    def forward(i):
        if i in STRAIGHT:
            corner[i].extend(along_x.pop((i, j)) for j in range(1, xs))
            corner[i].extend(along_y.pop((i, j)) for j in range(1, ys))
            return
        for j in range(1, xs):
            along_x[i, j].wait_recv()
            block = rows.at[i, y, xat(-j), 0]
            for k in range(1, ys):
                corner[i].append(send(block, block, device(z, yat(k), x)))
        for j in range(1, ys):
            along_y[i, j].wait_recv()
            block = rows.at[i, yat(-j), x, 1]
            for k in range(1, xs):
                corner[i].append(send(block, block, device(z, y, xat(k))))

    spots = ys * xs
    spread_to = [(j, k) for j in range(ys) for k in range(xs) if j or k][::-1]
    mine_lane = y * xs + x
    seen = set()

    def wait_once(name, copies):
        if name not in seen:
            seen.add(name)
            for copy in copies:
                copy.wait_recv()

    def compute(i):
        for copy in corner[i]:
            copy.wait_recv()
        wait_once("swap", swaps[:2])
        for j in range(ys):
            for k in range(xs):
                if (i, j, k) in side_waits:
                    side_waits[i, j, k].wait_recv()
        flat = [rows[i, :, :, h].reshape(spots * height, half) for h in range(2)]
        side = sides[i].reshape(spots * height, 2 * SIDE).astype(jnp.float32)
        lane = lax.broadcasted_iota(jnp.int32, side.shape, 1)
        hit = lax.rem(lane, SIDE) == mine_lane
        scale = jnp.sum(jnp.where(hit, side, 0.0), axis=1, keepdims=True)
        inner = []
        for share in range(2):
            left = jnp.dot(flat[0], gate[share, :half], preferred_element_type=jnp.float32)
            left += jnp.dot(flat[1], gate[share, half:], preferred_element_type=jnp.float32)
            right = jnp.dot(flat[0], up[share, :half], preferred_element_type=jnp.float32)
            right += jnp.dot(flat[1], up[share, half:], preferred_element_type=jnp.float32)
            inner.append((left / (1.0 + jnp.exp(-left)) * right).astype(low))
        wait_once("down", swaps[2:])
        ones[i] = []
        tile = math.gcd(half, 512)
        for h in range(2):
            for start in range(0, half, tile):
                cols = slice(h * half + start, h * half + start + tile)
                total = jnp.dot(inner[0], down[0, :, cols], preferred_element_type=jnp.float32)
                total += jnp.dot(inner[1], down[1, :, cols], preferred_element_type=jnp.float32)
                total = (total * scale).astype(low).reshape(ys, xs, height, tile)
                if h == 0:
                    part_a[i, :, :, :, start : start + tile] = total
                else:
                    for k in range(xs):
                        part_b[i, k, :, :, start : start + tile] = total[:, k]
            if i in GATHER:
                if True:
                    push(i, h)
            elif h == 0:
                for j in range(1, ys):
                    ones[i].append(send(part_a.at[i, yat(j)], first_a.at[i, j - 1], device(z, yat(j), x)))
            else:
                for j in range(1, xs):
                    ones[i].append(send(part_b.at[i, xat(j)], first_b.at[i, j - 1], device(z, y, xat(j))))

    def push(i, h):
        for index, (j, k) in enumerate(spread_to):
            src = part_a.at[i, yat(j), xat(k)] if h == 0 else part_b.at[i, xat(k), yat(j)]
            ones[i].append(send(src, direct.at[i, index, h], device(z, yat(j), xat(k))))

    def push_both(i):
        for h in range(2):
            push(i, h)

    def reduce(i):
        if i in GATHER:
            return
        twos[i] = []
        for copy in ones[i][: ys - 1]:
            copy.wait_recv()
        for k in range(1, xs):
            total = part_a[i, y, xat(k)].astype(jnp.float32)
            for j in range(1, ys):
                total += first_a[i, j - 1, xat(k)].astype(jnp.float32)
            send_a[i, k - 1] = total.astype(low)
            twos[i].append(send(send_a.at[i, k - 1], second_a.at[i, k - 1], device(z, y, xat(k))))
        for copy in ones[i][ys - 1 :]:
            copy.wait_recv()
        for k in range(1, ys):
            total = part_b[i, x, yat(k)].astype(jnp.float32)
            for j in range(1, xs):
                total += first_b[i, j - 1, yat(k)].astype(jnp.float32)
            send_b[i, k - 1] = total.astype(low)
            twos[i].append(send(send_b.at[i, k - 1], second_b.at[i, k - 1], device(z, yat(k), x)))

    def settle(i):
        for h in range(2):
            if i in GATHER:
                for copy in ones[i][h * (spots - 1) : (h + 1) * (spots - 1)]:
                    copy.wait_recv()
                total = (part_a[i, y, x] if h == 0 else part_b[i, x, y]).astype(jnp.float32)
                for index in range(spots - 1):
                    total += direct[i, index, h].astype(jnp.float32)
            elif h == 0:
                for copy in twos[i][: xs - 1]:
                    copy.wait_recv()
                total = part_a[i, y, x].astype(jnp.float32)
                for j in range(1, ys):
                    total += first_a[i, j - 1, x].astype(jnp.float32)
                for k in range(1, xs):
                    total += second_a[i, k - 1].astype(jnp.float32)
            else:
                for copy in twos[i][xs - 1 :]:
                    copy.wait_recv()
                total = part_b[i, x, y].astype(jnp.float32)
                for j in range(1, xs):
                    total += first_b[i, j - 1, y].astype(jnp.float32)
                for k in range(1, ys):
                    total += second_b[i, k - 1].astype(jnp.float32)
            if i:
                final[i - 1, h] = total.astype(low)
                ends[i, h] = send(final.at[i - 1, h], back.at[z, h], device(zat(i), y, x))
            else:
                back[z, h] = total.astype(low)

    for i in (1, 2, 3):
        arrive[i] = send(pack.at[zat(i)], rows.at[i, y, x], device(zat(i), y, x))
    rows[0, y, x] = pack[z]
    stages = {"s": spread, "f": forward, "c": compute, "p": push_both, "r": reduce, "e": settle}
    for name in ORDER:
        stages[name[0]](int(name[1:]))
    for h in range(2):
        for i in range(1, zs):
            if (i, h) in ends:
                ends[i, h].wait_recv()
        filled = back[:, h].reshape(slots, half)
        routed = jnp.dot(chosen, filled, preferred_element_type=jnp.float32)
        cols = slice(h * half, (h + 1) * half)
        out[:, cols] = (residual[:, cols].astype(jnp.float32) + routed).astype(out.dtype)
    for copy in used:
        copy.wait_send()


def run_layer(arrays, own, devices):
    (hidden, cache_keys, cache_values, lengths, first_gain, query_weight, key_weight, value_weight,
     mixing, head_gain, out_weight, second_gain, routes, route_weight) = arrays
    count, width = hidden.shape
    span = cache_keys.shape[1]
    zs = GROUPS
    chips = devices // (2 * zs)
    xs = math.isqrt(chips)
    ys = chips // xs
    experts = devices // EXP_SPLIT
    each = experts // zs
    capacity = max(2, 2 * count * TOP_K // experts)
    height = capacity * each // TOP_K
    half = width // 2
    inner = own[0].shape[2]
    low = jnp.bfloat16
    batch = math.gcd(count, 16)
    groups = count // batch
    sends = zs * ys * xs - 1 + 3 + 3 * (zs - 1) + zs * 4 * xs * ys
    vmem = pl.BlockSpec(memory_space=pltpu.VMEM)
    anywhere = pl.BlockSpec(memory_space=pltpu.HBM)
    small = [
        hidden, first_gain.reshape(1, -1), mixing.reshape(1, -1), head_gain.reshape(1, -1),
        second_gain.reshape(1, -1), routes.T, route_weight.T,
    ]
    return pl.pallas_call(
        functools.partial(layer_kernel, (zs, ys, xs), height, each),
        out_shape=(
            pltpu.VMEM((count, width), low),
            pltpu.VMEM((count, 2 * DK), low),
            pltpu.VMEM((count, DV), low),
        ),
        in_specs=[pl.BlockSpec(memory_space=pltpu.SMEM)] + [anywhere] * 16,
        out_specs=(vmem,) * 3,
        scratch_shapes=[
            *(pltpu.VMEM(array.shape, array.dtype) for array in small),
            pltpu.VMEM(cache_keys.shape, low),
            pltpu.VMEM(cache_values.shape, low),
            pltpu.VMEM(query_weight.shape, low),
            pltpu.VMEM((2, *key_weight.shape), low),
            pltpu.VMEM(out_weight.shape, low),
            pltpu.VMEM((count, 2 * HEADS, 2 * DK), jnp.float32),
            pltpu.VMEM((count, HEADS, DV), jnp.float32),
            pltpu.VMEM((2, count, DV), jnp.float32),
            pltpu.VMEM((count, HEADS, span), jnp.float32),
            pltpu.VMEM((count, HEADS, DV), jnp.float32),
            pltpu.VMEM((zs, 2, height, half), low),
            pltpu.VMEM((zs, height, 2 * SIDE), low),
            pltpu.VMEM((count, width), low),
            pltpu.VMEM((zs, ys, xs, 2, height, half), low),
            pltpu.VMEM((zs, ys, xs, height, 2 * SIDE), low),
            pltpu.VMEM((zs, ys, xs, height, half), low),
            pltpu.VMEM((zs, xs, ys, height, half), low),
            pltpu.VMEM((zs, max(1, ys - 1), xs, height, half), low),
            pltpu.VMEM((zs, max(1, xs - 1), ys, height, half), low),
            pltpu.VMEM((zs, max(1, xs - 1), height, half), low),
            pltpu.VMEM((zs, max(1, ys - 1), height, half), low),
            pltpu.VMEM((zs, max(1, xs - 1), height, half), low),
            pltpu.VMEM((zs, max(1, ys - 1), height, half), low),
            pltpu.VMEM((zs, max(1, ys * xs - 1), 2, height, half), low),
            pltpu.VMEM((zs - 1, 2, height, half), low),
            pltpu.VMEM((zs, 2, height, half), low),
            pltpu.VMEM((2, width, inner), low),
            pltpu.VMEM((2, width, inner), low),
            pltpu.VMEM((2, inner, width), low),
            pltpu.SemaphoreType.DMA((14,)),
            pltpu.SemaphoreType.DMA((groups,)),
            pltpu.SemaphoreType.DMA((groups,)),
            pltpu.SemaphoreType.DMA((sends,)),
            pltpu.SemaphoreType.DMA((sends,)),
        ],
        compiler_params=pltpu.CompilerParams(
            collective_id=0, has_side_effects=True, vmem_limit_bytes=60 * 1024 * 1024
        ),
        name="layer",
    )(
        lengths, hidden, cache_keys, cache_values, small[1], query_weight, key_weight, value_weight,
        small[2], small[3], out_weight, small[4], small[5], small[6], *own,
    )


def finish_kernel(*refs):
    count = len(refs) // 2
    sources, targets, sems = refs[:count], refs[count:-1], refs[-1]
    copies = [
        pltpu.make_async_copy(source, target, sems.at[index])
        for index, (source, target) in enumerate(zip(sources, targets))
    ]
    for copy in copies:
        copy.start()
    for copy in copies:
        copy.wait()


def finish(made):
    anywhere = pl.BlockSpec(memory_space=pl.ANY)
    return pl.pallas_call(
        finish_kernel,
        out_shape=tuple(jax.ShapeDtypeStruct(array.shape, array.dtype) for array in made),
        in_specs=[pl.BlockSpec(memory_space=pltpu.VMEM)] * len(made),
        out_specs=(anywhere,) * len(made),
        scratch_shapes=[pltpu.SemaphoreType.DMA((len(made),))],
        name="finish",
    )(*made)


def per_device(
    hidden,
    cache_keys,
    cache_values,
    lengths,
    first_gain,
    query_weight,
    key_weight,
    value_weight,
    mixing,
    head_gain,
    out_weight,
    second_gain,
    routes,
    route_weight,
    expert_gate,
    expert_up,
    expert_down,
):
    arrays = (
        hidden, cache_keys, cache_values, lengths, first_gain, query_weight, key_weight, value_weight,
        mixing, head_gain, out_weight, second_gain, routes, route_weight,
    )
    own = (expert_gate, expert_up, expert_down)
    made = run_layer(arrays, own, lax.axis_size("ep"))
    return finish([pltpu.with_memory_space_constraint(array, pltpu.VMEM) for array in made])


def solution(mesh):
    return jax.shard_map(
        per_device,
        mesh=mesh,
        in_specs=(
            P("ep", None),
            P("ep", None, None),
            P("ep", None, None),
            P("ep"),
            P(),
            P(),
            P(),
            P(),
            P(),
            P(),
            P(),
            P(),
            P("ep", None),
            P("ep", None),
            P("ep", None, None),
            P("ep", None, None),
            P("ep", None, None),
        ),
        out_specs=(P("ep", None), P("ep", None), P("ep", None)),
        check_vma=False,
    )
```

```python
import functools
import math

import jax
import jax.numpy as jnp
from jax import lax
from jax.experimental import pallas as pl
from jax.experimental.pallas import tpu as pltpu
from jax.sharding import PartitionSpec as P

D = 2048
HEADS = 8
DK = 64
DV = 128
EXP_SPLIT = 2
TOP_K = 4
GROUPS = 4
SIDE = 64
ORDER = ('s0', 's1', 'w0', 's2', 's3', 's6', 's7', 's4', 's5', 'c3', 'c2', 'e3', 'c1', 'e2', 'c0', 'e1', 'e0')
PIECE = 512


epsilon = 1e-06


def column(row):
    size = row.shape[1]
    down = lax.broadcasted_iota(jnp.int32, (size, size), 0)
    across = lax.broadcasted_iota(jnp.int32, (size, size), 1)
    return jnp.sum(jnp.where(down == across, row, jnp.zeros_like(row)), axis=1, keepdims=True)


def layer_kernel(dims, height, each, lengths_in, hidden_in, keys, values, first_gain_in, query_weight, key_weight,
                 value_weight, mixing_in, head_gain_in, out_weight, second_gain_in, routes_in, route_weight_in,
                 gate_own, up_own, down_own,
                 out, new_key, new_value,
                 hidden, first_gain, mixing, head_gain, second_gain, routes, route_weight,
                 lengths, key_buf, value_buf, query_buf, kv_buf, out_buf, queries, heads, fresh, contrast, owns,
                 pack, side_pack, residual, rows, sides, part, direct, final, back, gate, up, down,
                 load_sems, key_sems, value_sems, send_sems, recv_sems):
    zs, ys, xs = dims
    count, width = hidden.shape
    half = width // 2
    span = keys.shape[1]
    groups = key_sems.shape[0]
    batch = count // groups
    low = jnp.bfloat16
    me = lax.axis_index("ep")
    c = lax.rem(me, 2)
    x = lax.rem(me // 2, xs)
    y = lax.rem(me // (2 * xs), ys)
    z = me // (2 * xs * ys)

    def device(pz, py, px):
        return ((pz * ys + py) * xs + px) * 2 + c

    def zat(i):
        flip = z
        if i % 2:
            flip = flip + 1 - 2 * lax.rem(flip, 2)
        if i // 2:
            flip = lax.rem(flip + 2, 4)
        return flip

    def yat(j):
        return lax.rem(y + j + ys, ys)

    def xat(j):
        return lax.rem(x + j + xs, xs)

    used = []

    def send(src, dst, target):
        index = len(used)
        copy = pltpu.make_async_remote_copy(
            src_ref=src,
            dst_ref=dst,
            send_sem=send_sems.at[index],
            recv_sem=recv_sems.at[index],
            device_id=(target,),
            device_id_type=pl.DeviceIdType.MESH,
        )
        copy.start()
        used.append(copy)
        return copy

    moves = []
    for src, dst in (
        (hidden_in, hidden), (first_gain_in, first_gain), (routes_in, routes), (route_weight_in, route_weight),
        (mixing_in, mixing), (head_gain_in, head_gain), (second_gain_in, second_gain), (lengths_in, lengths),
        (query_weight, query_buf), (key_weight, kv_buf.at[0]), (value_weight, kv_buf.at[1]),
        (gate_own.at[0], gate.at[0]), (up_own.at[0], up.at[0]), (down_own.at[0], down.at[0]),
    ):
        moves.append(pltpu.make_async_copy(src, dst, load_sems.at[len(moves)]))
    small, query_move, kv_moves, own_moves = moves[:8], moves[8], moves[9:11], moves[11:]
    piece = math.gcd(width, PIECE)
    out_moves = [
        pltpu.make_async_copy(
            out_weight.at[:, pl.ds(start, piece)], out_buf.at[:, pl.ds(start, piece)],
            load_sems.at[len(moves) + start // piece],
        )
        for start in range(0, width, piece)
    ]

    def fetch(source, target, flags, step):
        at = pl.ds(step * batch, batch)
        return pltpu.make_async_copy(source.at[at], target.at[at], flags.at[step])

    def fetch_keys(step):
        return fetch(keys, key_buf, key_sems, step)

    def fetch_values(step):
        return fetch(values, value_buf, value_sems, step)

    for copy in (*small, query_move, *kv_moves):
        copy.start()

    def begin_keys(step, carry):
        fetch_keys(step).start()
        return carry

    def begin_values(step, carry):
        fetch_values(step).start()
        return carry

    lax.fori_loop(0, groups, begin_keys, 0)
    lax.fori_loop(0, groups, begin_values, 0)
    for copy in (*out_moves, *own_moves):
        copy.start()

    others = [
        (i, j, k) for i in range(zs) for j in range(ys) for k in range(xs) if (i, j, k) != (0, 0, 0)
    ]
    sibling = me + 1 - 2 * c
    barrier = pltpu.get_barrier_semaphore()
    for i, j, k in others:
        pl.semaphore_signal(
            barrier, inc=1, device_id=(device(zat(i), yat(j), xat(k)),), device_id_type=pl.DeviceIdType.MESH
        )
    pl.semaphore_signal(barrier, inc=1, device_id=(sibling,), device_id_type=pl.DeviceIdType.MESH)

    for copy in small:
        copy.wait()
    group = column(routes[:1, :]) // each
    down_at = lax.broadcasted_iota(jnp.int32, (count, count), 0)
    across = lax.broadcasted_iota(jnp.int32, (count, count), 1)
    other = routes[:1, :] // each
    before = jnp.where((group == other) & (across < down_at), 1, 0)
    target = group * height + jnp.sum(before, axis=1, keepdims=True)
    slots = zs * height
    chosen = target == lax.broadcasted_iota(jnp.int32, (count, slots), 1)
    chosen = jnp.where(chosen, 1.0, 0.0).astype(low)
    place = lax.broadcasted_iota(jnp.int32, (count, SIDE), 1)
    scale = jnp.zeros((count, SIDE), jnp.float32)
    for k in range(routes.shape[0]):
        inside = column(routes[k : k + 1, :]) - group * each
        scale += jnp.where(place == inside, column(route_weight[k : k + 1, :]), 0.0)
    high = scale.astype(low)
    side = jnp.concatenate([high, (scale - high.astype(jnp.float32)).astype(low)], axis=1)
    turned = (((0,), (0,)), ((), ()))
    packed = lax.dot_general(chosen, side, turned, preferred_element_type=jnp.float32)
    side_pack[...] = packed.astype(low).reshape(zs, height, 2 * SIDE)
    sides[0, y, x] = side_pack[z]

    entry = hidden[...].astype(jnp.float32)
    factor = lax.rsqrt(jnp.mean(entry * entry, axis=-1, keepdims=True) + epsilon)
    normed = (entry * factor * first_gain[...]).astype(low)
    lane = lax.broadcasted_iota(jnp.int32, (count, 2 * DK), 1)
    query_move.wait()
    query = jnp.dot(normed, query_buf[...], preferred_element_type=jnp.float32)
    query = query.astype(low).astype(jnp.float32)
    for head in range(HEADS):
        block = query[:, head * 2 * DK : (head + 1) * 2 * DK]
        queries[:, head, :] = jnp.where(lane < DK, block, 0.0)
        queries[:, HEADS + head, :] = jnp.where(lane < DK, 0.0, block)
    for index, result in ((0, new_key), (1, new_value)):
        kv_moves[index].wait()
        made = jnp.dot(normed, kv_buf[index], preferred_element_type=jnp.float32).astype(low)
        result[...] = made
        fresh[index] = made.astype(jnp.float32)

    position = lax.broadcasted_iota(jnp.int32, (1, span), 1)
    mixes = column(mixing[...])

    def weigh(step, carry):
        fetch_keys(step).wait()
        for offset in range(batch):
            s = step * batch + offset
            wide = queries[s]
            own_key = fresh[0, pl.ds(s, 1), :]
            scores = lax.dot_general(
                wide.astype(low),
                key_buf[s],
                (((1,), (1,)), ((), ())),
                preferred_element_type=jnp.float32,
            ) * DK ** (-0.5)
            own = jnp.sum(wide * own_key, axis=-1, keepdims=True) * DK ** (-0.5)
            scores = jnp.where(position < lengths[s], scores, -jnp.inf)
            highest = jnp.maximum(jnp.max(scores, axis=-1, keepdims=True), own)
            weights = jnp.exp(scores - highest)
            own = jnp.exp(own - highest)
            inverse = 1.0 / (jnp.sum(weights, axis=-1, keepdims=True) + own)
            first, second = inverse[:HEADS], inverse[HEADS:] * mixes
            contrast[s] = weights[:HEADS] * first - weights[HEADS:] * second
            own = (own[:HEADS] * first - own[HEADS:] * second).astype(low).astype(jnp.float32)
            owns[s] = own * fresh[1, pl.ds(s, 1), :]
        return carry

    lax.fori_loop(0, groups, weigh, 0)

    pl.semaphore_wait(barrier, len(others) + 1)
    side_waits = {}
    for i, j, k in others:
        side_waits[i, j, k] = send(side_pack.at[zat(i)], sides.at[i, y, x], device(zat(i), yat(j), xat(k)))

    def mix(step, carry):
        fetch_values(step).wait()
        for offset in range(batch):
            s = step * batch + offset
            mixed = jnp.dot(contrast[s].astype(low), value_buf[s], preferred_element_type=jnp.float32)
            mixed += owns[s]
            scale = lax.rsqrt(jnp.mean(mixed * mixed, axis=-1, keepdims=True) + epsilon)
            heads[s] = mixed * scale * head_gain[...]
        return carry

    lax.fori_loop(0, groups, mix, 0)

    joined = jnp.concatenate([heads[:, head, :] for head in range(HEADS)], axis=1).astype(low)
    for index, copy in enumerate(out_moves):
        cols = slice(index * piece, (index + 1) * piece)
        copy.wait()
        update = jnp.dot(joined, out_buf[:, cols], preferred_element_type=jnp.float32)
        residual[:, cols] = (hidden[:, cols].astype(jnp.float32) + update).astype(low)
    kept = residual[...].astype(jnp.float32)
    factor = lax.rsqrt(jnp.mean(kept * kept, axis=-1, keepdims=True) + epsilon)
    inputs = (kept * factor * second_gain[...]).astype(low)
    for h in range(2):
        packed = lax.dot_general(
            chosen, inputs[:, h * half : (h + 1) * half], turned, preferred_element_type=jnp.float32
        )
        pack[:, h] = packed.astype(low).reshape(zs, height, half)

    arrive, spread_waits, gather_waits, ends = {}, {}, {}, {}
    spots = ys * xs
    spread_to = [(j, k) for j in range(ys) for k in range(xs) if j or k][::-1]
    mine_lane = y * xs + x
    swaps = []
    seen = set()

    def swap(_):
        for copy, (whole, mine) in zip(own_moves, ((gate, gate.at[0]), (up, up.at[0]), (down, down.at[0]))):
            copy.wait()
            swaps.append(send(mine, whole.at[1], sibling))

    def wait_once(name, copies):
        if name not in seen:
            seen.add(name)
            for copy in copies:
                copy.wait_recv()

    def spread(code):
        i, h = divmod(code, 2)
        if i:
            arrive[i, h].wait_recv()
        block = rows.at[i, y, x, h]
        spread_waits[i, h] = [send(block, block, device(z, yat(j), xat(k))) for j, k in spread_to]

    def compute(i):
        for h in range(2):
            for copy in spread_waits[i, h]:
                copy.wait_recv()
        wait_once("swap", swaps[:2])
        for j in range(ys):
            for k in range(xs):
                if (i, j, k) in side_waits:
                    side_waits[i, j, k].wait_recv()
        flat = [rows[i, :, :, h].reshape(spots * height, half) for h in range(2)]
        side = sides[i].reshape(spots * height, 2 * SIDE).astype(jnp.float32)
        lane = lax.broadcasted_iota(jnp.int32, side.shape, 1)
        hit = lax.rem(lane, SIDE) == mine_lane
        scale = jnp.sum(jnp.where(hit, side, 0.0), axis=1, keepdims=True)
        inner = []
        for share in range(2):
            left = jnp.dot(flat[0], gate[share, :half], preferred_element_type=jnp.float32)
            left += jnp.dot(flat[1], gate[share, half:], preferred_element_type=jnp.float32)
            right = jnp.dot(flat[0], up[share, :half], preferred_element_type=jnp.float32)
            right += jnp.dot(flat[1], up[share, half:], preferred_element_type=jnp.float32)
            inner.append((left / (1.0 + jnp.exp(-left)) * right).astype(low))
        wait_once("down", swaps[2:])
        tile = math.gcd(half, 512)
        for h in range(2):
            for start in range(0, half, tile):
                cols = slice(h * half + start, h * half + start + tile)
                total = jnp.dot(inner[0], down[0, :, cols], preferred_element_type=jnp.float32)
                total += jnp.dot(inner[1], down[1, :, cols], preferred_element_type=jnp.float32)
                total = (total * scale).astype(low).reshape(ys, xs, height, tile)
                part[i, h, :, :, :, start : start + tile] = total
            gather_waits[i, h] = [
                send(part.at[i, h, yat(j), xat(k)], direct.at[i, h, index], device(z, yat(j), xat(k)))
                for index, (j, k) in enumerate(spread_to)
            ]

    def settle(i):
        for h in range(2):
            for copy in gather_waits[i, h]:
                copy.wait_recv()
            total = part[i, h, y, x].astype(jnp.float32)
            for index in range(spots - 1):
                total += direct[i, h, index].astype(jnp.float32)
            if i:
                final[i - 1, h] = total.astype(low)
                ends[i, h] = send(final.at[i - 1, h], back.at[z, h], device(zat(i), y, x))
            else:
                back[z, h] = total.astype(low)

    for i, h in ((1, 0), (1, 1), (3, 0), (3, 1), (2, 0), (2, 1)):
        if i:
            arrive[i, h] = send(pack.at[zat(i), h], rows.at[i, y, x, h], device(zat(i), y, x))
    rows[0, y, x] = pack[z]
    stages = {"w": swap, "s": spread, "c": compute, "e": settle}
    for name in ORDER:
        stages[name[0]](int(name[1:]))
    for h in range(2):
        for i in range(1, zs):
            ends[i, h].wait_recv()
        filled = back[:, h].reshape(slots, half)
        routed = jnp.dot(chosen, filled, preferred_element_type=jnp.float32)
        cols = slice(h * half, (h + 1) * half)
        out[:, cols] = (residual[:, cols].astype(jnp.float32) + routed).astype(out.dtype)
    for copy in used:
        copy.wait_send()


def run_layer(arrays, own, devices):
    (hidden, cache_keys, cache_values, lengths, first_gain, query_weight, key_weight, value_weight,
     mixing, head_gain, out_weight, second_gain, routes, route_weight) = arrays
    count, width = hidden.shape
    span = cache_keys.shape[1]
    zs = GROUPS
    chips = devices // (2 * zs)
    xs = math.isqrt(chips)
    ys = chips // xs
    experts = devices // EXP_SPLIT
    each = experts // zs
    capacity = max(2, 2 * count * TOP_K // experts)
    height = capacity * each // TOP_K
    half = width // 2
    inner = own[0].shape[2]
    low = jnp.bfloat16
    batch = math.gcd(count, 16)
    groups = count // batch
    sends = zs * ys * xs - 1 + 3 + 4 * (zs - 1) + 4 * zs * (ys * xs - 1)
    vmem = pl.BlockSpec(memory_space=pltpu.VMEM)
    anywhere = pl.BlockSpec(memory_space=pltpu.HBM)
    small = [
        hidden, first_gain.reshape(1, -1), mixing.reshape(1, -1), head_gain.reshape(1, -1),
        second_gain.reshape(1, -1), routes.T, route_weight.T,
    ]
    return pl.pallas_call(
        functools.partial(layer_kernel, (zs, ys, xs), height, each),
        out_shape=(
            pltpu.VMEM((count, width), low),
            pltpu.VMEM((count, 2 * DK), low),
            pltpu.VMEM((count, DV), low),
        ),
        in_specs=[anywhere] * 17,
        out_specs=(vmem,) * 3,
        scratch_shapes=[
            *(pltpu.VMEM(array.shape, array.dtype) for array in small),
            pltpu.SMEM(lengths.shape, lengths.dtype),
            pltpu.VMEM(cache_keys.shape, low),
            pltpu.VMEM(cache_values.shape, low),
            pltpu.VMEM(query_weight.shape, low),
            pltpu.VMEM((2, *key_weight.shape), low),
            pltpu.VMEM(out_weight.shape, low),
            pltpu.VMEM((count, 2 * HEADS, 2 * DK), jnp.float32),
            pltpu.VMEM((count, HEADS, DV), jnp.float32),
            pltpu.VMEM((2, count, DV), jnp.float32),
            pltpu.VMEM((count, HEADS, span), jnp.float32),
            pltpu.VMEM((count, HEADS, DV), jnp.float32),
            pltpu.VMEM((zs, 2, height, half), low),
            pltpu.VMEM((zs, height, 2 * SIDE), low),
            pltpu.VMEM((count, width), low),
            pltpu.VMEM((zs, ys, xs, 2, height, half), low),
            pltpu.VMEM((zs, ys, xs, height, 2 * SIDE), low),
            pltpu.VMEM((zs, 2, ys, xs, height, half), low),
            pltpu.VMEM((zs, 2, max(1, ys * xs - 1), height, half), low),
            pltpu.VMEM((zs - 1, 2, height, half), low),
            pltpu.VMEM((zs, 2, height, half), low),
            pltpu.VMEM((2, width, inner), low),
            pltpu.VMEM((2, width, inner), low),
            pltpu.VMEM((2, inner, width), low),
            pltpu.SemaphoreType.DMA((14 + width // math.gcd(width, PIECE),)),
            pltpu.SemaphoreType.DMA((groups,)),
            pltpu.SemaphoreType.DMA((groups,)),
            pltpu.SemaphoreType.DMA((sends,)),
            pltpu.SemaphoreType.DMA((sends,)),
        ],
        compiler_params=pltpu.CompilerParams(
            collective_id=0, has_side_effects=True, vmem_limit_bytes=60 * 1024 * 1024
        ),
        name="layer",
    )(
        lengths, hidden, cache_keys, cache_values, small[1], query_weight, key_weight, value_weight,
        small[2], small[3], out_weight, small[4], small[5], small[6], *own,
    )


def finish_kernel(*refs):
    count = len(refs) // 2
    sources, targets, sems = refs[:count], refs[count:-1], refs[-1]
    copies = [
        pltpu.make_async_copy(source, target, sems.at[index])
        for index, (source, target) in enumerate(zip(sources, targets))
    ]
    for copy in copies:
        copy.start()
    for copy in copies:
        copy.wait()


def finish(made):
    anywhere = pl.BlockSpec(memory_space=pl.ANY)
    return pl.pallas_call(
        finish_kernel,
        out_shape=tuple(jax.ShapeDtypeStruct(array.shape, array.dtype) for array in made),
        in_specs=[pl.BlockSpec(memory_space=pltpu.VMEM)] * len(made),
        out_specs=(anywhere,) * len(made),
        scratch_shapes=[pltpu.SemaphoreType.DMA((len(made),))],
        name="finish",
    )(*made)


def per_device(
    hidden,
    cache_keys,
    cache_values,
    lengths,
    first_gain,
    query_weight,
    key_weight,
    value_weight,
    mixing,
    head_gain,
    out_weight,
    second_gain,
    routes,
    route_weight,
    expert_gate,
    expert_up,
    expert_down,
):
    arrays = (
        hidden, cache_keys, cache_values, lengths, first_gain, query_weight, key_weight, value_weight,
        mixing, head_gain, out_weight, second_gain, routes, route_weight,
    )
    own = (expert_gate, expert_up, expert_down)
    made = run_layer(arrays, own, lax.axis_size("ep"))
    return finish([pltpu.with_memory_space_constraint(array, pltpu.VMEM) for array in made])


def solution(mesh):
    return jax.shard_map(
        per_device,
        mesh=mesh,
        in_specs=(
            P("ep", None),
            P("ep", None, None),
            P("ep", None, None),
            P("ep"),
            P(),
            P(),
            P(),
            P(),
            P(),
            P(),
            P(),
            P(),
            P("ep", None),
            P("ep", None),
            P("ep", None, None),
            P("ep", None, None),
            P("ep", None, None),
        ),
        out_specs=(P("ep", None), P("ep", None), P("ep", None)),
        check_vma=False,
    )
```

```python
import functools
import math

import jax
import jax.numpy as jnp
from jax import lax
from jax.experimental import pallas as pl
from jax.experimental.pallas import tpu as pltpu
from jax.sharding import PartitionSpec as P

D = 2048
HEADS = 8
DK = 64
DV = 128
EXP_SPLIT = 2
TOP_K = 4
GROUPS = 4
SIDE = 64
ORDER = ('s0', 's1', 'w0', 's2', 's3', 's6', 's7', 's4', 's5', 'c3', 'c2', 'e3', 'c1', 'e2', 'c0', 'e1', 'e0')
PIECE = 1024


epsilon = 1e-06


def column(row):
    size = row.shape[1]
    down = lax.broadcasted_iota(jnp.int32, (size, size), 0)
    across = lax.broadcasted_iota(jnp.int32, (size, size), 1)
    return jnp.sum(jnp.where(down == across, row, jnp.zeros_like(row)), axis=1, keepdims=True)


def layer_kernel(dims, height, each, lengths_in, hidden_in, keys, values, first_gain_in, query_weight, key_weight,
                 value_weight, mixing_in, head_gain_in, out_weight, second_gain_in, routes_in, route_weight_in,
                 gate_own, up_own, down_own,
                 out, new_key, new_value,
                 hidden, first_gain, mixing, head_gain, second_gain, routes, route_weight,
                 lengths, key_buf, value_buf, query_buf, kv_buf, out_buf, queries, heads, fresh, contrast, owns,
                 pack, side_pack, residual, rows, sides, part, direct, final, back, gate, up, down,
                 load_sems, key_sems, value_sems, send_sems, recv_sems):
    zs, ys, xs = dims
    count, width = hidden.shape
    half = width // 2
    span = keys.shape[1]
    groups = key_sems.shape[0]
    batch = count // groups
    low = jnp.bfloat16
    me = lax.axis_index("ep")
    c = lax.rem(me, 2)
    x = lax.rem(me // 2, xs)
    y = lax.rem(me // (2 * xs), ys)
    z = me // (2 * xs * ys)

    def device(pz, py, px):
        return ((pz * ys + py) * xs + px) * 2 + c

    def zat(i):
        flip = z
        if i % 2:
            flip = flip + 1 - 2 * lax.rem(flip, 2)
        if i // 2:
            flip = lax.rem(flip + 2, 4)
        return flip

    def yat(j):
        return lax.rem(y + j + ys, ys)

    def xat(j):
        return lax.rem(x + j + xs, xs)

    used = []

    def send(src, dst, target):
        index = len(used)
        copy = pltpu.make_async_remote_copy(
            src_ref=src,
            dst_ref=dst,
            send_sem=send_sems.at[index],
            recv_sem=recv_sems.at[index],
            device_id=(target,),
            device_id_type=pl.DeviceIdType.MESH,
        )
        copy.start()
        used.append(copy)
        return copy

    moves = []
    for src, dst in (
        (hidden_in, hidden), (first_gain_in, first_gain), (routes_in, routes), (route_weight_in, route_weight),
        (mixing_in, mixing), (head_gain_in, head_gain), (second_gain_in, second_gain), (lengths_in, lengths),
        (query_weight, query_buf), (key_weight, kv_buf.at[0]), (value_weight, kv_buf.at[1]),
        (gate_own.at[0], gate.at[0]), (up_own.at[0], up.at[0]), (down_own.at[0], down.at[0]),
    ):
        moves.append(pltpu.make_async_copy(src, dst, load_sems.at[len(moves)]))
    small, query_move, kv_moves, own_moves = moves[:8], moves[8], moves[9:11], moves[11:]
    piece = math.gcd(width, PIECE)
    out_moves = [
        pltpu.make_async_copy(
            out_weight.at[:, pl.ds(start, piece)], out_buf.at[:, pl.ds(start, piece)],
            load_sems.at[len(moves) + start // piece],
        )
        for start in range(0, width, piece)
    ]

    def fetch(source, target, flags, step):
        size = count // flags.shape[0]
        at = pl.ds(step * size, size)
        return pltpu.make_async_copy(source.at[at], target.at[at], flags.at[step])

    def fetch_keys(step):
        return fetch(keys, key_buf, key_sems, step)

    def fetch_values(step):
        return fetch(values, value_buf, value_sems, step)

    for copy in (*small, query_move, *kv_moves):
        copy.start()

    def begin_keys(step, carry):
        fetch_keys(step).start()
        return carry

    def begin_values(step, carry):
        fetch_values(step).start()
        return carry

    lax.fori_loop(0, groups, begin_keys, 0)
    lax.fori_loop(0, value_sems.shape[0], begin_values, 0)
    for copy in (*out_moves, *own_moves):
        copy.start()

    others = [
        (i, j, k) for i in range(zs) for j in range(ys) for k in range(xs) if (i, j, k) != (0, 0, 0)
    ]
    sibling = me + 1 - 2 * c
    barrier = pltpu.get_barrier_semaphore()
    for i, j, k in others:
        pl.semaphore_signal(
            barrier, inc=1, device_id=(device(zat(i), yat(j), xat(k)),), device_id_type=pl.DeviceIdType.MESH
        )
    pl.semaphore_signal(barrier, inc=1, device_id=(sibling,), device_id_type=pl.DeviceIdType.MESH)

    for copy in small:
        copy.wait()
    group = column(routes[:1, :]) // each
    down_at = lax.broadcasted_iota(jnp.int32, (count, count), 0)
    across = lax.broadcasted_iota(jnp.int32, (count, count), 1)
    other = routes[:1, :] // each
    before = jnp.where((group == other) & (across < down_at), 1, 0)
    target = group * height + jnp.sum(before, axis=1, keepdims=True)
    slots = zs * height
    chosen = target == lax.broadcasted_iota(jnp.int32, (count, slots), 1)
    chosen = jnp.where(chosen, 1.0, 0.0).astype(low)
    place = lax.broadcasted_iota(jnp.int32, (count, SIDE), 1)
    scale = jnp.zeros((count, SIDE), jnp.float32)
    for k in range(routes.shape[0]):
        inside = column(routes[k : k + 1, :]) - group * each
        scale += jnp.where(place == inside, column(route_weight[k : k + 1, :]), 0.0)
    high = scale.astype(low)
    side = jnp.concatenate([high, (scale - high.astype(jnp.float32)).astype(low)], axis=1)
    turned = (((0,), (0,)), ((), ()))
    packed = lax.dot_general(chosen, side, turned, preferred_element_type=jnp.float32)
    side_pack[...] = packed.astype(low).reshape(zs, height, 2 * SIDE)
    sides[0, y, x] = side_pack[z]

    entry = hidden[...].astype(jnp.float32)
    factor = lax.rsqrt(jnp.mean(entry * entry, axis=-1, keepdims=True) + epsilon)
    normed = (entry * factor * first_gain[...]).astype(low)
    lane = lax.broadcasted_iota(jnp.int32, (count, 2 * DK), 1)
    query_move.wait()
    query = jnp.dot(normed, query_buf[...], preferred_element_type=jnp.float32)
    query = query.astype(low).astype(jnp.float32)
    for head in range(HEADS):
        block = query[:, head * 2 * DK : (head + 1) * 2 * DK]
        queries[:, head, :] = jnp.where(lane < DK, block, 0.0)
        queries[:, HEADS + head, :] = jnp.where(lane < DK, 0.0, block)
    for index, result in ((0, new_key), (1, new_value)):
        kv_moves[index].wait()
        made = jnp.dot(normed, kv_buf[index], preferred_element_type=jnp.float32).astype(low)
        result[...] = made
        fresh[index] = made.astype(jnp.float32)

    position = lax.broadcasted_iota(jnp.int32, (1, span), 1)
    mixes = column(mixing[...])

    def weigh(step, carry):
        fetch_keys(step).wait()
        for offset in range(batch):
            s = step * batch + offset
            wide = queries[s]
            own_key = fresh[0, pl.ds(s, 1), :]
            scores = lax.dot_general(
                wide.astype(low),
                key_buf[s],
                (((1,), (1,)), ((), ())),
                preferred_element_type=jnp.float32,
            ) * DK ** (-0.5)
            own = jnp.sum(wide * own_key, axis=-1, keepdims=True) * DK ** (-0.5)
            scores = jnp.where(position < lengths[s], scores, -jnp.inf)
            highest = jnp.maximum(jnp.max(scores, axis=-1, keepdims=True), own)
            weights = jnp.exp(scores - highest)
            own = jnp.exp(own - highest)
            inverse = 1.0 / (jnp.sum(weights, axis=-1, keepdims=True) + own)
            first, second = inverse[:HEADS], inverse[HEADS:] * mixes
            contrast[s] = weights[:HEADS] * first - weights[HEADS:] * second
            own = (own[:HEADS] * first - own[HEADS:] * second).astype(low).astype(jnp.float32)
            owns[s] = own * fresh[1, pl.ds(s, 1), :]
        return carry

    lax.fori_loop(0, groups, weigh, 0)

    pl.semaphore_wait(barrier, len(others) + 1)
    side_waits = {}
    for i, j, k in others:
        side_waits[i, j, k] = send(side_pack.at[zat(i)], sides.at[i, y, x], device(zat(i), yat(j), xat(k)))

    def mix(step, carry):
        fetch_values(step).wait()
        size = count // value_sems.shape[0]
        for offset in range(size):
            s = step * size + offset
            mixed = jnp.dot(contrast[s].astype(low), value_buf[s], preferred_element_type=jnp.float32)
            mixed += owns[s]
            scale = lax.rsqrt(jnp.mean(mixed * mixed, axis=-1, keepdims=True) + epsilon)
            heads[s] = mixed * scale * head_gain[...]
        return carry

    lax.fori_loop(0, value_sems.shape[0], mix, 0)

    joined = jnp.concatenate([heads[:, head, :] for head in range(HEADS)], axis=1).astype(low)
    for index, copy in enumerate(out_moves):
        cols = slice(index * piece, (index + 1) * piece)
        copy.wait()
        update = jnp.dot(joined, out_buf[:, cols], preferred_element_type=jnp.float32)
        residual[:, cols] = (hidden[:, cols].astype(jnp.float32) + update).astype(low)
    kept = residual[...].astype(jnp.float32)
    factor = lax.rsqrt(jnp.mean(kept * kept, axis=-1, keepdims=True) + epsilon)
    inputs = (kept * factor * second_gain[...]).astype(low)
    for h in range(2):
        packed = lax.dot_general(
            chosen, inputs[:, h * half : (h + 1) * half], turned, preferred_element_type=jnp.float32
        )
        pack[:, h] = packed.astype(low).reshape(zs, height, half)

    arrive, spread_waits, gather_waits, ends = {}, {}, {}, {}
    spots = ys * xs
    spread_to = [(j, k) for j in range(ys) for k in range(xs) if j or k][::-1]
    mine_lane = y * xs + x
    swaps = []
    seen = set()

    def swap(_):
        for copy, (whole, mine) in zip(own_moves, ((gate, gate.at[0]), (up, up.at[0]), (down, down.at[0]))):
            copy.wait()
            swaps.append(send(mine, whole.at[1], sibling))

    def wait_once(name, copies):
        if name not in seen:
            seen.add(name)
            for copy in copies:
                copy.wait_recv()

    def spread(code):
        i, h = divmod(code, 2)
        if i:
            arrive[i, h].wait_recv()
        block = rows.at[i, y, x, h]
        spread_waits[i, h] = [send(block, block, device(z, yat(j), xat(k))) for j, k in spread_to]

    def compute(i):
        for h in range(2):
            for copy in spread_waits[i, h]:
                copy.wait_recv()
        wait_once("swap", swaps[:2])
        for j in range(ys):
            for k in range(xs):
                if (i, j, k) in side_waits:
                    side_waits[i, j, k].wait_recv()
        flat = [rows[i, :, :, h].reshape(spots * height, half) for h in range(2)]
        side = sides[i].reshape(spots * height, 2 * SIDE).astype(jnp.float32)
        lane = lax.broadcasted_iota(jnp.int32, side.shape, 1)
        hit = lax.rem(lane, SIDE) == mine_lane
        scale = jnp.sum(jnp.where(hit, side, 0.0), axis=1, keepdims=True)
        inner = []
        for share in range(2):
            left = jnp.dot(flat[0], gate[share, :half], preferred_element_type=jnp.float32)
            left += jnp.dot(flat[1], gate[share, half:], preferred_element_type=jnp.float32)
            right = jnp.dot(flat[0], up[share, :half], preferred_element_type=jnp.float32)
            right += jnp.dot(flat[1], up[share, half:], preferred_element_type=jnp.float32)
            inner.append((left / (1.0 + jnp.exp(-left)) * right).astype(low))
        wait_once("down", swaps[2:])
        tile = math.gcd(half, 512)
        for h in range(2):
            for start in range(0, half, tile):
                cols = slice(h * half + start, h * half + start + tile)
                total = jnp.dot(inner[0], down[0, :, cols], preferred_element_type=jnp.float32)
                total += jnp.dot(inner[1], down[1, :, cols], preferred_element_type=jnp.float32)
                total = (total * scale).astype(low).reshape(ys, xs, height, tile)
                part[i, h, :, :, :, start : start + tile] = total
            gather_waits[i, h] = [
                send(part.at[i, h, yat(j), xat(k)], direct.at[i, h, index], device(z, yat(j), xat(k)))
                for index, (j, k) in enumerate(spread_to)
            ]

    def settle(i):
        for h in range(2):
            for copy in gather_waits[i, h]:
                copy.wait_recv()
            total = part[i, h, y, x].astype(jnp.float32)
            for index in range(spots - 1):
                total += direct[i, h, index].astype(jnp.float32)
            if i:
                final[i - 1, h] = total.astype(low)
                ends[i, h] = send(final.at[i - 1, h], back.at[z, h], device(zat(i), y, x))
            else:
                back[z, h] = total.astype(low)

    for i, h in ((1, 0), (1, 1), (3, 0), (3, 1), (2, 0), (2, 1)):
        if i:
            arrive[i, h] = send(pack.at[zat(i), h], rows.at[i, y, x, h], device(zat(i), y, x))
    rows[0, y, x] = pack[z]
    stages = {"w": swap, "s": spread, "c": compute, "e": settle}
    for name in ORDER:
        stages[name[0]](int(name[1:]))
    for h in range(2):
        for i in range(1, zs):
            ends[i, h].wait_recv()
        filled = back[:, h].reshape(slots, half)
        routed = jnp.dot(chosen, filled, preferred_element_type=jnp.float32)
        cols = slice(h * half, (h + 1) * half)
        out[:, cols] = (residual[:, cols].astype(jnp.float32) + routed).astype(out.dtype)
    for copy in used:
        copy.wait_send()


def run_layer(arrays, own, devices):
    (hidden, cache_keys, cache_values, lengths, first_gain, query_weight, key_weight, value_weight,
     mixing, head_gain, out_weight, second_gain, routes, route_weight) = arrays
    count, width = hidden.shape
    span = cache_keys.shape[1]
    zs = GROUPS
    chips = devices // (2 * zs)
    xs = math.isqrt(chips)
    ys = chips // xs
    experts = devices // EXP_SPLIT
    each = experts // zs
    capacity = max(2, 2 * count * TOP_K // experts)
    height = capacity * each // TOP_K
    half = width // 2
    inner = own[0].shape[2]
    low = jnp.bfloat16
    batch = math.gcd(count, 16)
    groups = count // batch
    sends = zs * ys * xs - 1 + 3 + 4 * (zs - 1) + 4 * zs * (ys * xs - 1)
    vmem = pl.BlockSpec(memory_space=pltpu.VMEM)
    anywhere = pl.BlockSpec(memory_space=pltpu.HBM)
    small = [
        hidden, first_gain.reshape(1, -1), mixing.reshape(1, -1), head_gain.reshape(1, -1),
        second_gain.reshape(1, -1), routes.T, route_weight.T,
    ]
    return pl.pallas_call(
        functools.partial(layer_kernel, (zs, ys, xs), height, each),
        out_shape=(
            pltpu.VMEM((count, width), low),
            pltpu.VMEM((count, 2 * DK), low),
            pltpu.VMEM((count, DV), low),
        ),
        in_specs=[anywhere] * 17,
        out_specs=(vmem,) * 3,
        scratch_shapes=[
            *(pltpu.VMEM(array.shape, array.dtype) for array in small),
            pltpu.SMEM(lengths.shape, lengths.dtype),
            pltpu.VMEM(cache_keys.shape, low),
            pltpu.VMEM(cache_values.shape, low),
            pltpu.VMEM(query_weight.shape, low),
            pltpu.VMEM((2, *key_weight.shape), low),
            pltpu.VMEM(out_weight.shape, low),
            pltpu.VMEM((count, 2 * HEADS, 2 * DK), jnp.float32),
            pltpu.VMEM((count, HEADS, DV), jnp.float32),
            pltpu.VMEM((2, count, DV), jnp.float32),
            pltpu.VMEM((count, HEADS, span), jnp.float32),
            pltpu.VMEM((count, HEADS, DV), jnp.float32),
            pltpu.VMEM((zs, 2, height, half), low),
            pltpu.VMEM((zs, height, 2 * SIDE), low),
            pltpu.VMEM((count, width), low),
            pltpu.VMEM((zs, ys, xs, 2, height, half), low),
            pltpu.VMEM((zs, ys, xs, height, 2 * SIDE), low),
            pltpu.VMEM((zs, 2, ys, xs, height, half), low),
            pltpu.VMEM((zs, 2, max(1, ys * xs - 1), height, half), low),
            pltpu.VMEM((zs - 1, 2, height, half), low),
            pltpu.VMEM((zs, 2, height, half), low),
            pltpu.VMEM((2, width, inner), low),
            pltpu.VMEM((2, width, inner), low),
            pltpu.VMEM((2, inner, width), low),
            pltpu.SemaphoreType.DMA((14 + width // math.gcd(width, PIECE),)),
            pltpu.SemaphoreType.DMA((groups,)),
            pltpu.SemaphoreType.DMA((count // math.gcd(count, 16),)),
            pltpu.SemaphoreType.DMA((sends,)),
            pltpu.SemaphoreType.DMA((sends,)),
        ],
        compiler_params=pltpu.CompilerParams(
            collective_id=0, has_side_effects=True, vmem_limit_bytes=60 * 1024 * 1024
        ),
        name="layer",
    )(
        lengths, hidden, cache_keys, cache_values, small[1], query_weight, key_weight, value_weight,
        small[2], small[3], out_weight, small[4], small[5], small[6], *own,
    )


def finish_kernel(*refs):
    count = len(refs) // 2
    sources, targets, sems = refs[:count], refs[count:-1], refs[-1]
    copies = [
        pltpu.make_async_copy(source, target, sems.at[index])
        for index, (source, target) in enumerate(zip(sources, targets))
    ]
    for copy in copies:
        copy.start()
    for copy in copies:
        copy.wait()


def finish(made):
    anywhere = pl.BlockSpec(memory_space=pl.ANY)
    return pl.pallas_call(
        finish_kernel,
        out_shape=tuple(jax.ShapeDtypeStruct(array.shape, array.dtype) for array in made),
        in_specs=[pl.BlockSpec(memory_space=pltpu.VMEM)] * len(made),
        out_specs=(anywhere,) * len(made),
        scratch_shapes=[pltpu.SemaphoreType.DMA((len(made),))],
        name="finish",
    )(*made)


def per_device(
    hidden,
    cache_keys,
    cache_values,
    lengths,
    first_gain,
    query_weight,
    key_weight,
    value_weight,
    mixing,
    head_gain,
    out_weight,
    second_gain,
    routes,
    route_weight,
    expert_gate,
    expert_up,
    expert_down,
):
    arrays = (
        hidden, cache_keys, cache_values, lengths, first_gain, query_weight, key_weight, value_weight,
        mixing, head_gain, out_weight, second_gain, routes, route_weight,
    )
    own = (expert_gate, expert_up, expert_down)
    made = run_layer(arrays, own, lax.axis_size("ep"))
    return finish([pltpu.with_memory_space_constraint(array, pltpu.VMEM) for array in made])


def solution(mesh):
    return jax.shard_map(
        per_device,
        mesh=mesh,
        in_specs=(
            P("ep", None),
            P("ep", None, None),
            P("ep", None, None),
            P("ep"),
            P(),
            P(),
            P(),
            P(),
            P(),
            P(),
            P(),
            P(),
            P("ep", None),
            P("ep", None),
            P("ep", None, None),
            P("ep", None, None),
            P("ep", None, None),
        ),
        out_specs=(P("ep", None), P("ep", None), P("ep", None)),
        check_vma=False,
    )
```
